32 devices in a mesh: grp: 2 (over y), fs: 4 (over z), tp: 4 (over x, core).
Axes of the slice: x: 2, y: 2, z: 4, core: 2. Of those that a mesh axis runs over, the one named last changes fastest.
Arguments:
- tokens: bfloat16 [1024, 2048], P(('grp', 'fs')), parts along dimension 0, may hold values from -12 to 12, as said below
- mix_heads: bfloat16 [1024, 2048], P(('grp', 'fs'), 'tp'), parts along dimension 0, may hold values from -6 to 6
- norm_first: float32 [2048], replicated, may hold values from 0.1 to 1.9
- gate_first: bfloat16 [2048, 5632], P('fs', 'tp'), may hold values from -0.125 to 0.125
- up_first: bfloat16 [2048, 5632], P('fs', 'tp'), may hold values from -0.125 to 0.125
- down_first: bfloat16 [5632, 2048], P('tp', 'fs'), may hold values from -0.078125 to 0.078125
- out_weight: bfloat16 [2048, 2048], P('tp', 'fs'), may hold values from -0.125 to 0.125
- norm_second: float32 [2048], replicated, may hold values from 0.1 to 1.9
- gate_second: bfloat16 [2048, 5632], P('fs', 'tp'), may hold values from -0.125 to 0.125
- up_second: bfloat16 [2048, 5632], P('fs', 'tp'), may hold values from -0.125 to 0.125
- down_second: bfloat16 [5632, 2048], P('tp', 'fs'), may hold values from -0.078125 to 0.078125
Outputs:
- layer_out: bfloat16 [1024, 2048], P(('grp', 'fs')), parts along dimension 0
The draws below stay inside these ranges and needn't reach their ends.
There are 2 independent parts, one for each index of `grp`. The reference program is written for one: setup_inputs(seed, part) draws one part's arguments, and reference() takes and returns one part's arrays. A program takes and returns all parts, laid end to end along the dimension named above; an argument that names none is the same for every part. Nothing has to cross between parts.
Inputs may be any that keep to these rules, and one draw needn't show every extreme that they name: Each row of tokens carries a scale of its own.
All inputs are finite; a program needn't handle non-finite values.
Results may differ from the reference program's by a relative error of at most 0.014.
Values may be sent and summed in bfloat16 or wider, within the bound.
A program may use at most 64 MiB of HBM per device.

```python
import math
import jax
import jax.numpy as jnp
from jax import lax

D = 2048
FF = 5632
MIX = 2048
TOKENS = 512
N_TP = 4


def draw_tokens(key, part):
    subkeys = jax.random.split(key, 3)
    base_values = jax.random.normal(subkeys[0], (TOKENS, D), jnp.float32)
    row_scale = jnp.exp(jax.random.uniform(subkeys[1], (TOKENS, 1), jnp.float32, math.log(0.4), math.log(2.5)))
    values = base_values * row_scale
    return jnp.clip(values, -12.0, 12.0).astype(jnp.bfloat16)


def levels(key, dims, cuts, smallest, largest):
    loudness, own = 1.0, jax.random.fold_in(key, 6)
    for position, shards_of in cuts:
        steps = jnp.exp(jax.random.uniform(jax.random.fold_in(own, position), (shards_of,), jnp.float32, smallest / len(cuts), largest / len(cuts)))
        loudness = loudness * jnp.repeat(steps, dims[position] // shards_of).reshape([-1 if axis == position else 1 for axis in range(len(dims))])
    return loudness


def centred(stream_key, dims, deviation, most, cuts=(), dtype=jnp.bfloat16):
    level = levels(stream_key, dims, cuts, -0.22, 0.18) if cuts else 1.0
    entries = jax.random.normal(stream_key, dims, jnp.float32) * deviation * level
    return jnp.minimum(jnp.maximum(entries, -most), most).astype(dtype)


def setup_inputs(seed: int = 0, part: int = 0) -> dict:
    keys = jax.random.split(jax.random.key(seed), 12)
    part_keys = jax.random.split(jax.random.fold_in(keys[11], part), 12)
    return {
        "tokens": draw_tokens(jax.random.fold_in(jax.random.fold_in(keys[11], part), 71), part),
        "mix_heads": centred(part_keys[1], (TOKENS, MIX), 1.0, 6.0, ((0, 4), (1, 4))),
        "norm_first": jnp.clip(1.0 + 0.18 * jax.random.normal(keys[2], (D,), jnp.float32), 0.1, 1.9),
        "gate_first": centred(keys[3], (D, FF), D ** -0.5, 0.125, ((0, 4), (1, 4))),
        "up_first": centred(keys[4], (D, FF), D ** -0.5, 0.125, ((0, 4), (1, 4))),
        "down_first": centred(keys[5], (FF, D), FF ** -0.5, 0.078125, ((0, 4), (1, 4))),
        "out_weight": centred(keys[6], (MIX, D), MIX ** -0.5, 0.125, ((0, 4), (1, 4))),
        "norm_second": jnp.clip(1.0 + 0.18 * jax.random.normal(keys[7], (D,), jnp.float32), 0.1, 1.9),
        "gate_second": centred(keys[8], (D, FF), D ** -0.5, 0.125, ((0, 4), (1, 4))),
        "up_second": centred(keys[9], (D, FF), D ** -0.5, 0.125, ((0, 4), (1, 4))),
        "down_second": centred(keys[10], (FF, D), FF ** -0.5, 0.078125, ((0, 4), (1, 4))),
    }


EPS = 0.1

def norm_rows(row_block, gain_vector):
    widened = row_block.astype(jnp.float32)
    scaled = widened * lax.rsqrt(lax.optimization_barrier(jnp.mean(widened * widened, axis=-1, keepdims=True)) + EPS)
    return (scaled * gain_vector.astype(jnp.float32)).astype(jnp.bfloat16)

def branch_terms(normed, gate_weight, value_weight, down_weight, added_term):
    block_width = FF // N_TP

    def block_term(index):
        first_col = (index * block_width).astype(jnp.int32)
        gates = jnp.dot(normed, lax.dynamic_slice_in_dim(gate_weight, first_col, block_width, 1), preferred_element_type=jnp.float32)
        values = jnp.dot(normed, lax.dynamic_slice_in_dim(value_weight, first_col, block_width, 1), preferred_element_type=jnp.float32)
        hidden = (jax.nn.silu(gates) * values).astype(jnp.bfloat16)
        partial_value = 0.5 * jnp.dot(hidden, lax.dynamic_slice_in_dim(down_weight, first_col, block_width, 0), preferred_element_type=jnp.float32)
        return partial_value + added_term(index)

    def accumulate(index, total):
        rounded = lax.optimization_barrier(block_term(index).astype(jnp.bfloat16))
        return total + rounded.astype(jnp.float32)
    start_total = jnp.zeros((normed.shape[0], down_weight.shape[1]), jnp.float32)
    return lax.fori_loop(0, N_TP, accumulate, start_total)

def reference(tokens, mix_heads, norm_first, gate_first, up_first, down_first, out_weight, norm_second, gate_second, up_second, down_second):
    head_width = MIX // N_TP

    def head_term(index):
        first_col = (index * head_width).astype(jnp.int32)
        heads = lax.dynamic_slice_in_dim(mix_heads, first_col, head_width, 1)
        weight_rows = lax.dynamic_slice_in_dim(out_weight, first_col, head_width, 0)
        return jnp.dot(heads, weight_rows, preferred_element_type=jnp.float32)

    def no_term(index):
        return jnp.zeros((tokens.shape[0], tokens.shape[1]), jnp.float32)
    normed_one = norm_rows(tokens, norm_first)
    mixed_sum = branch_terms(normed_one, gate_first, up_first, down_first, head_term)
    resid_two = tokens.astype(jnp.float32) + mixed_sum
    normed_two = norm_rows(resid_two, norm_second)
    ffn_sum = branch_terms(normed_two, gate_second, up_second, down_second, no_term)
    return (resid_two + ffn_sum).astype(jnp.bfloat16)
```

```python
import functools

import jax
import jax.numpy as jnp
from jax import lax
from jax.experimental import pallas as pl
from jax.experimental.pallas import tpu as pltpu
from jax.sharding import PartitionSpec as P

EPS = 0.1
MESH = pl.DeviceIdType.MESH
BF16 = jnp.bfloat16
F32 = jnp.float32


def loop(count, body):
    def step(i, carry):
        body(i)
        return carry

    lax.fori_loop(0, count, step, 0)


def kernel(n_fs, n_tp, chunk,
           tok, mix, gain1, wg1, wu1, wd1, wo, gain2, wg2, wu2, wd2,
           out,
           vg1, vu1, vd1, vo, vg2, vu2, vd2,
           norm_rows, raw, nb1, nb2, mixed, grads, sums, in1, in2, hid1, hid2,
           terms, got1, got2, resid, squares, done_rows, joined,
           wsem, p0_send, p0_recv, raw_send, raw_recv, mix_send, mix_recv,
           rs_send, rs_recv, ag_send, ag_recv, tp_send, tp_recv,
           sq_send, sq_recv, nrm_send, nrm_recv, out_send, out_recv):
    f, t = lax.axis_index("fs"), lax.axis_index("tp")
    rows_in, width = tok.shape
    total = rows_in * n_fs
    share = total // n_tp
    half = total // 2
    n_chunks = half // chunk
    dc = width // n_fs

    weights = ((wg1, vg1), (wu1, vu1), (wd1, vd1), (wo, vo), (wg2, vg2), (wu2, vu2), (wd2, vd2))
    loads = [pltpu.make_async_copy(a, b, wsem.at[i]) for i, (a, b) in enumerate(weights)]
    for load in loads:
        load.start()

    barrier = pltpu.get_barrier_semaphore()

    def greet(i):
        pf, pt = i // n_tp, i % n_tp

        @pl.when(jnp.logical_or(pf != f, pt != t))
        def _():
            pl.semaphore_signal(barrier, inc=1, device_id={"fs": pf, "tp": pt}, device_id_type=MESH)

    loop(n_fs * n_tp, greet)

    def cols(j):
        return pl.ds(pl.multiple_of(j * dc, dc), dc)

    def block(j, size):
        return pl.ds(pl.multiple_of(j * size, size), size)

    def remote(src, dst, send, recv, **where):
        return pltpu.make_async_remote_copy(
            src_ref=src, dst_ref=dst, send_sem=send, recv_sem=recv,
            device_id=where, device_id_type=MESH)

    def norm_piece(i):
        rows = block(i, 32)
        x = tok[rows, :].astype(F32)
        scaled = x * lax.rsqrt(jnp.mean(x * x, axis=-1, keepdims=True) + EPS)
        norm_rows[rows, :] = (scaled * gain1[...]).astype(BF16)

    loop(rows_in // 32, norm_piece)
    pl.semaphore_wait(barrier, n_fs * n_tp - 1)

    def p0_copy(j, slot):
        return remote(norm_rows.at[:, cols(j)], nb1.at[block(slot, rows_in), :],
                      p0_send.at[j], p0_recv.at[slot], fs=j)

    def raw_copy(j):
        return remote(tok.at[:, cols(j)], raw, raw_send.at[j], raw_recv, fs=j)

    def mix_copy(slot, side, where):
        place = mixed.at[block(slot, rows_in), :]
        return remote(place, place, mix_send.at[slot, side], mix_recv.at[slot], fs=where)

    def p0_start(i):
        j = (f + 1 + i) % n_fs
        p0_copy(j, f).start()

    loop(n_fs - 1, p0_start)
    nb1[block(f, rows_in), :] = norm_rows[:, cols(f)]
    mixed[block(f, rows_in), :] = mix[...]

    @pl.when(f == t)
    def _():
        def raw_start(i):
            raw_copy((f + 1 + i) % n_fs).start()

        loop(n_fs - 1, raw_start)
        raw[...] = tok[:, cols(f)]

    def gates(nb, vg, vu, before):
        def piece(i):
            j = (f + i) % n_fs
            before(j)
            rows = block(j, rows_in)
            x = nb[rows, :]
            grads[0, rows, :] = jnp.dot(x, vg[...], preferred_element_type=F32)
            grads[1, rows, :] = jnp.dot(x, vu[...], preferred_element_type=F32)

        loop(n_fs, piece)

    def chain(layer, arrived, hid, with_mix):
        def side_of(side):
            hops = (n_fs - 1 - f) if side == 0 else f
            toward = (f - 1) if side == 0 else (f + 1)
            away = (f + 1) if side == 0 else (f - 1)
            return hops, toward, away

        def rows_of(side, c):
            return pl.ds(pl.multiple_of(side * half + c * chunk, chunk), chunk)

        def rs_copy(side, c, where):
            rows = rows_of(side, c)
            return remote(sums.at[:, rows, :], arrived.at[:, rows, :],
                          rs_send.at[layer, side, c], rs_recv.at[layer, side, c], fs=where)

        def ag_copy(side, c, where):
            rows = rows_of(side, c)
            return remote(hid.at[rows, :], hid.at[rows, :],
                          ag_send.at[layer, side, c], ag_recv.at[layer, side, c], fs=where)

        def step(s):
            for side in (0, 1):
                hops, toward, away = side_of(side)
                c = s - hops

                @pl.when(jnp.logical_and(c >= 0, c < n_chunks))
                def _():
                    rows = rows_of(side, c)

                    @pl.when(hops == 0)
                    def _():
                        sums[:, rows, :] = grads[:, rows, :].astype(BF16)
                        rs_copy(side, c, toward).start()

                    @pl.when(hops > 0)
                    def _():
                        rs_copy(side, c, f).wait_recv()

                    @pl.when(jnp.logical_and(hops > 0, hops < n_fs - 1))
                    def _():
                        sums[:, rows, :] = (grads[:, rows, :] + arrived[:, rows, :].astype(F32)).astype(BF16)
                        rs_copy(side, c, toward).start()

                    @pl.when(hops == n_fs - 1)
                    def _():
                        g = grads[0, rows, :] + arrived[0, rows, :].astype(F32)
                        v = grads[1, rows, :] + arrived[1, rows, :].astype(F32)
                        hid[rows, :] = (g / (1.0 + jnp.exp(-g)) * v).astype(BF16)
                        ag_copy(side, c, away).start()

            for side in (0, 1):
                hops, toward, away = side_of(side)
                dist = n_fs - 1 - hops
                c = s - (n_fs - 1) - dist

                @pl.when(jnp.logical_and(dist > 0, jnp.logical_and(c >= 0, c < n_chunks)))
                def _():
                    ag_copy(side, c, f).wait_recv()

                    @pl.when(dist < n_fs - 1)
                    def _():
                        ag_copy(side, c, away).start()

            if with_mix:
                @pl.when(s < n_fs)
                def _():
                    low, high = f - s, f + s

                    @pl.when(low >= 0)
                    def _():
                        @pl.when(s > 0)
                        def _():
                            mix_copy(low, 0, f).wait_recv()

                        @pl.when(f < n_fs - 1)
                        def _():
                            mix_copy(low, 0, f + 1).start()

                    @pl.when(high < n_fs)
                    def _():
                        @pl.when(s > 0)
                        def _():
                            mix_copy(high, 1, f).wait_recv()

                        @pl.when(f > 0)
                        def _():
                            mix_copy(high, 1, f - 1).start()

        loop(n_chunks + 2 * (n_fs - 1), step)

        def drain(c):
            for side in (0, 1):
                hops, toward, away = side_of(side)

                @pl.when(hops < n_fs - 1)
                def _():
                    rs_copy(side, c, f).wait_send()

                @pl.when(hops > 0)
                def _():
                    ag_copy(side, c, f).wait_send()

        loop(n_chunks, drain)

    def tp_copy(layer, j, slot, got):
        return remote(terms.at[block(j, share), :], got.at[slot],
                      tp_send.at[layer, j], tp_recv.at[layer, slot], tp=j)

    def reduce_tp(layer, hid, vd, got, start_value, with_mix):
        def piece(i):
            j = (t + 1 + i) % n_tp
            rows = block(j, share)
            value = 0.5 * jnp.dot(hid[rows, :], vd[...], preferred_element_type=F32)
            if with_mix:
                value = value + jnp.dot(mixed[rows, :], vo[...], preferred_element_type=F32)
            terms[rows, :] = value.astype(BF16)

            @pl.when(i < n_tp - 1)
            def _():
                tp_copy(layer, j, t, got).start()

        loop(n_tp, piece)
        resid[...] = start_value + terms[block(t, share), :].astype(F32)

        def add(i):
            j = (t + 1 + i) % n_tp
            tp_copy(layer, j, j, got).wait_recv()
            resid[...] = resid[...] + got[j].astype(F32)

        loop(n_tp - 1, add)

        def drain(i):
            j = (t + 1 + i) % n_tp
            tp_copy(layer, j, t, got).wait_send()

        loop(n_tp - 1, drain)

    loads[0].wait()
    loads[1].wait()

    def need_rows(j):
        @pl.when(j != f)
        def _():
            p0_copy(j, j).wait_recv()

    gates(nb1, vg1, vu1, need_rows)
    chain(0, in1, hid1, True)
    loads[2].wait()
    loads[3].wait()

    @pl.when(f != t)
    def _():
        raw_copy(f).wait_recv()

    reduce_tp(0, hid1, vd1, got1, raw[...].astype(F32), True)

    def sq_copy(j, slot):
        return remote(squares.at[f], squares.at[slot], sq_send.at[j], sq_recv.at[slot], fs=j)

    x = resid[...]
    own = jnp.sum(x * x, axis=-1, keepdims=True)
    squares[f] = jnp.transpose(jnp.broadcast_to(own, (share, 128)))[0:8, :]

    def sq_start(i):
        sq_copy((f + 1 + i) % n_fs, f).start()

    def sq_wait(i):
        j = (f + 1 + i) % n_fs
        sq_copy(j, j).wait_recv()

    loop(n_fs - 1, sq_start)
    loop(n_fs - 1, sq_wait)
    summed = squares[0]
    for j in range(1, n_fs):
        summed = summed + squares[j]
    mean = jnp.transpose(jnp.broadcast_to(summed[0:1, :], (128, share)))[:, 0:1] * (1.0 / width)
    nb2[block(t, share), :] = (resid[...] * lax.rsqrt(mean + EPS) * gain2[:, cols(f)]).astype(BF16)

    def nrm_copy(j, slot):
        place = nb2.at[block(slot, share), :]
        return remote(place, place, nrm_send.at[j], nrm_recv.at[slot], tp=j)

    def nrm_start(i):
        nrm_copy((t + 1 + i) % n_tp, t).start()

    def nrm_wait(i):
        j = (t + 1 + i) % n_tp
        nrm_copy(j, j).wait_recv()

    loop(n_tp - 1, nrm_start)
    loads[4].wait()
    loads[5].wait()
    loop(n_tp - 1, nrm_wait)
    gates(nb2, vg2, vu2, lambda j: None)
    chain(1, in2, hid2, False)
    loads[6].wait()
    reduce_tp(1, hid2, vd2, got2, resid[...], False)
    done_rows[...] = resid[...].astype(BF16)

    def out_copy(j, slot):
        return remote(done_rows, joined.at[:, cols(slot)], out_send.at[j], out_recv.at[slot], fs=t, tp=j)

    def out_start(i):
        j = (t + i) % n_tp

        @pl.when(jnp.logical_or(f != t, j != t))
        def _():
            out_copy(j, f).start()

    loop(n_tp, out_start)

    @pl.when(f == t)
    def _():
        joined[:, cols(f)] = done_rows[...]

    def out_wait(j):
        @pl.when(jnp.logical_or(f != t, j != f))
        def _():
            out_copy(t, j).wait_recv()

    loop(n_fs, out_wait)
    out[...] = joined[...]

    def last_fs(i):
        j = (f + 1 + i) % n_fs
        p0_copy(j, f).wait_send()
        sq_copy(j, f).wait_send()

        @pl.when(f == t)
        def _():
            raw_copy(j).wait_send()

    loop(n_fs - 1, last_fs)

    def last_mix(j):
        @pl.when(jnp.logical_and(j <= f, f < n_fs - 1))
        def _():
            mix_copy(j, 0, f).wait_send()

        @pl.when(jnp.logical_and(j >= f, f > 0))
        def _():
            mix_copy(j, 1, f).wait_send()

    loop(n_fs, last_mix)

    def last_tp(i):
        nrm_copy((t + 1 + i) % n_tp, t).wait_send()

    loop(n_tp - 1, last_tp)

    def last_out(j):
        @pl.when(jnp.logical_or(f != t, j != t))
        def _():
            out_copy(j, f).wait_send()

    loop(n_tp, last_out)


def solution(mesh):
    n_fs, n_tp = mesh.shape["fs"], mesh.shape["tp"]

    def local(tokens, mix_heads, norm_first, gate_first, up_first, down_first, out_weight,
              norm_second, gate_second, up_second, down_second):
        rows_in, width = tokens.shape
        total = rows_in * n_fs
        share = total // n_tp
        dc, hidden = gate_first.shape
        heads = mix_heads.shape[1]
        chunk = rows_in // 4
        n_chunks = total // 2 // chunk
        dma = pltpu.SemaphoreType.DMA
        vmem = pl.BlockSpec(memory_space=pltpu.VMEM)
        hbm = pl.BlockSpec(memory_space=pl.ANY)
        return pl.pallas_call(
            functools.partial(kernel, n_fs, n_tp, chunk),
            out_shape=jax.ShapeDtypeStruct((rows_in, width), BF16),
            in_specs=[vmem, vmem, vmem, hbm, hbm, hbm, hbm, vmem, hbm, hbm, hbm],
            out_specs=vmem,
            scratch_shapes=[
                pltpu.VMEM(gate_first.shape, BF16),
                pltpu.VMEM(up_first.shape, BF16),
                pltpu.VMEM(down_first.shape, BF16),
                pltpu.VMEM(out_weight.shape, BF16),
                pltpu.VMEM(gate_second.shape, BF16),
                pltpu.VMEM(up_second.shape, BF16),
                pltpu.VMEM(down_second.shape, BF16),
                pltpu.VMEM((rows_in, width), BF16),
                pltpu.VMEM((rows_in, dc), BF16),
                pltpu.VMEM((total, dc), BF16),
                pltpu.VMEM((total, dc), BF16),
                pltpu.VMEM((total, heads), BF16),
                pltpu.VMEM((2, total, hidden), F32),
                pltpu.VMEM((2, total, hidden), BF16),
                pltpu.VMEM((2, total, hidden), BF16),
                pltpu.VMEM((2, total, hidden), BF16),
                pltpu.VMEM((total, hidden), BF16),
                pltpu.VMEM((total, hidden), BF16),
                pltpu.VMEM((total, dc), BF16),
                pltpu.VMEM((n_tp, share, dc), BF16),
                pltpu.VMEM((n_tp, share, dc), BF16),
                pltpu.VMEM((share, dc), F32),
                pltpu.VMEM((n_fs, 8, share), F32),
                pltpu.VMEM((share, dc), BF16),
                pltpu.VMEM((rows_in, width), BF16),
                dma((7,)), dma((n_fs,)), dma((n_fs,)), dma((n_fs,)), dma,
                dma((n_fs, 2)), dma((n_fs,)),
                dma((2, 2, n_chunks)), dma((2, 2, n_chunks)), dma((2, 2, n_chunks)), dma((2, 2, n_chunks)),
                dma((2, n_tp)), dma((2, n_tp)),
                dma((n_fs,)), dma((n_fs,)), dma((n_tp,)), dma((n_tp,)), dma((n_tp,)), dma((n_fs,)),
            ],
            compiler_params=pltpu.CompilerParams(
                collective_id=0, has_side_effects=True, vmem_limit_bytes=60 * 1024 * 1024),
        )(tokens, mix_heads, norm_first.reshape(1, -1), gate_first, up_first, down_first, out_weight,
          norm_second.reshape(1, -1), gate_second, up_second, down_second)

    in_specs = (
        P(("grp", "fs"), None),
        P(("grp", "fs"), "tp"),
        P(),
        P("fs", "tp"),
        P("fs", "tp"),
        P("tp", "fs"),
        P("tp", "fs"),
        P(),
        P("fs", "tp"),
        P("fs", "tp"),
        P("tp", "fs"),
    )
    return jax.shard_map(local, mesh=mesh, in_specs=in_specs, out_specs=P(("grp", "fs"), None), check_vma=False)
```

```python
import functools

import jax
import jax.numpy as jnp
from jax import lax
from jax.experimental import pallas as pl
from jax.experimental.pallas import tpu as pltpu
from jax.sharding import PartitionSpec as P

EPS = 0.1
MESH = pl.DeviceIdType.MESH
BF16 = jnp.bfloat16
F32 = jnp.float32


def loop(count, body):
    def step(i, carry):
        body(i)
        return carry

    lax.fori_loop(0, count, step, 0)


def kernel(n_fs, n_tp, chunk,
           tok, mix, gain1, wg1, wu1, wd1, wo, gain2, wg2, wu2, wd2,
           out,
           vg1, vu1, vd1, vo, vg2, vu2, vd2,
           raw, nb2, mixed, grads, sums, in1, in2, hid1, hid2,
           terms, got1, got2, resid, squares1, squares, done_rows, joined,
           wsem, p0_send, p0_recv, fw_send, fw_recv, s1_send, s1_recv, mix_send, mix_recv,
           rs_send, rs_recv, ag_send, ag_recv, tp_send, tp_recv,
           sq_send, sq_recv, nrm_send, nrm_recv, nfw_send, nfw_recv,
           out_send, out_recv, ofw_send, ofw_recv):
    f, t = lax.axis_index("fs"), lax.axis_index("tp")
    rows_in, width = tok.shape
    total = rows_in * n_fs
    share = total // n_tp
    half = total // 2
    n_chunks = half // chunk
    dc = width // n_fs

    weights = ((wg1, vg1), (wu1, vu1), (wd1, vd1), (wo, vo), (wg2, vg2), (wu2, vu2), (wd2, vd2))
    loads = [pltpu.make_async_copy(a, b, wsem.at[i]) for i, (a, b) in enumerate(weights)]
    for load in loads:
        load.start()

    barrier = pltpu.get_barrier_semaphore()

    def greet(i):
        pf, pt = i // n_tp, i % n_tp

        @pl.when(jnp.logical_or(pf != f, pt != t))
        def _():
            pl.semaphore_signal(barrier, inc=1, device_id={"fs": pf, "tp": pt}, device_id_type=MESH)

    loop(n_fs * n_tp, greet)

    def cols(j):
        return pl.ds(pl.multiple_of(j * dc, dc), dc)

    def block(j, size):
        return pl.ds(pl.multiple_of(j * size, size), size)

    def remote(src, dst, send, recv, **where):
        return pltpu.make_async_remote_copy(
            src_ref=src, dst_ref=dst, send_sem=send, recv_sem=recv,
            device_id=where, device_id_type=MESH)

    c_own = t % 2
    partner = t + 1 - 2 * c_own
    half_in = rows_in // 2
    n_pairs = n_tp // 2

    def squares_of(x):
        own = jnp.sum(x * x, axis=-1, keepdims=True)
        return jnp.transpose(jnp.broadcast_to(own, (x.shape[0], 128)))[0:8, :]

    def scale_of(summed):
        column = jnp.transpose(jnp.broadcast_to(summed[0:1, :], (128, summed.shape[1])))[:, 0:1]
        return lax.rsqrt(column * (1.0 / width) + EPS)

    def piece_of(slot):
        return pl.ds(pl.multiple_of(slot * rows_in + c_own * half_in, half_in), half_in)

    def p0_copy(j, slot):
        return remote(tok.at[block(c_own, half_in), cols(j)], raw.at[piece_of(slot), :],
                      p0_send.at[j], p0_recv.at[slot], fs=j)

    def fw_copy(slot):
        place = raw.at[piece_of(slot), :]
        return remote(place, place, fw_send.at[slot], fw_recv.at[slot], tp=partner)

    def s1_copy(j, slot):
        return remote(squares1.at[f], squares1.at[slot], s1_send.at[j], s1_recv.at[slot], fs=j)

    def sq_copy(j, slot):
        return remote(squares.at[f], squares.at[slot], sq_send.at[j], sq_recv.at[slot], fs=j)

    def mix_copy(slot, side, where):
        place = mixed.at[block(slot, rows_in), :]
        return remote(place, place, mix_send.at[slot, side], mix_recv.at[slot], fs=where)

    mixed[block(f, rows_in), :] = mix[...]
    pl.semaphore_wait(barrier, n_fs * n_tp - 1)

    def p0_start(i):
        p0_copy((f + 1 + i) % n_fs, f).start()

    loop(n_fs - 1, p0_start)
    squares1[f] = squares_of(tok[...].astype(F32))

    def s1_start(i):
        s1_copy((f + 1 + i) % n_fs, f).start()

    loop(n_fs - 1, s1_start)

    @pl.when(f < n_fs - 1)
    def _():
        mix_copy(f, 0, f + 1).start()

    @pl.when(f > 0)
    def _():
        mix_copy(f, 1, f - 1).start()

    raw[block(f, rows_in), :] = tok[:, cols(f)]

    def gates_one(j):
        rows = block(j, rows_in)
        x = (raw[rows, :].astype(F32) * scale_of(squares1[j]) * gain1[:, cols(f)]).astype(BF16)
        grads[0, rows, :] = jnp.dot(x, vg1[...], preferred_element_type=F32)
        grads[1, rows, :] = jnp.dot(x, vu1[...], preferred_element_type=F32)

    def side_of(side):
        hops = jnp.where(side == 0, n_fs - 1 - f, f)
        toward = jnp.where(side == 0, f - 1, f + 1)
        away = jnp.where(side == 0, f + 1, f - 1)
        return hops, toward, away

    near = jnp.where(2 * f >= n_fs, 0, 1)

    def chain(layer, arrived, hid, with_mix):
        def rows_of(side, c):
            return pl.ds(pl.multiple_of(side * half + c * chunk, chunk), chunk)

        def rs_copy(side, c, where):
            rows = rows_of(side, c)
            return remote(sums.at[:, rows, :], arrived.at[:, rows, :],
                          rs_send.at[layer, side, c], rs_recv.at[layer, side, c], fs=where)

        def ag_copy(side, c, where):
            rows = rows_of(side, c)
            return remote(hid.at[rows, :], hid.at[rows, :],
                          ag_send.at[layer, side, c], ag_recv.at[layer, side, c], fs=where)

        for side in (0, 1):
            hops, toward, away = side_of(side)

            @pl.when(hops == 0)
            def _():
                def first(c):
                    rows = rows_of(side, c)
                    sums[:, rows, :] = grads[:, rows, :].astype(BF16)
                    rs_copy(side, c, toward).start()

                loop(n_chunks, first)

        def step(s):
            for k in (0, 1):
                side = near if k == 0 else 1 - near
                hops, toward, away = side_of(side)
                c = s - hops

                @pl.when(jnp.logical_and(hops > 0, jnp.logical_and(c >= 0, c < n_chunks)))
                def _():
                    rows = rows_of(side, c)
                    rs_copy(side, c, f).wait_recv()

                    @pl.when(hops < n_fs - 1)
                    def _():
                        sums[:, rows, :] = (grads[:, rows, :] + arrived[:, rows, :].astype(F32)).astype(BF16)
                        rs_copy(side, c, toward).start()

                    @pl.when(hops == n_fs - 1)
                    def _():
                        g = grads[0, rows, :] + arrived[0, rows, :].astype(F32)
                        v = grads[1, rows, :] + arrived[1, rows, :].astype(F32)
                        hid[rows, :] = (g / (1.0 + jnp.exp(-g)) * v).astype(BF16)
                        ag_copy(side, c, away).start()

            if with_mix:
                @pl.when(jnp.logical_and(s > 0, s < n_fs))
                def _():
                    low, high = f - s, f + s

                    @pl.when(low >= 0)
                    def _():
                        mix_copy(low, 0, f).wait_recv()

                        @pl.when(f < n_fs - 1)
                        def _():
                            mix_copy(low, 0, f + 1).start()

                    @pl.when(high < n_fs)
                    def _():
                        mix_copy(high, 1, f).wait_recv()

                        @pl.when(f > 0)
                        def _():
                            mix_copy(high, 1, f - 1).start()

        loop(n_chunks + n_fs - 1, step)

        def relay(c):
            for k in (0, 1):
                side = 1 - near if k == 0 else near
                hops, toward, away = side_of(side)

                @pl.when(hops < n_fs - 1)
                def _():
                    ag_copy(side, c, f).wait_recv()

                    @pl.when(hops > 0)
                    def _():
                        ag_copy(side, c, away).start()

        def drain(c):
            for side in (0, 1):
                hops, toward, away = side_of(side)

                @pl.when(hops < n_fs - 1)
                def _():
                    rs_copy(side, c, f).wait_send()

                @pl.when(hops > 0)
                def _():
                    ag_copy(side, c, f).wait_send()

        return relay, lambda: loop(n_chunks, drain)

    def tp_copy(layer, j, slot, got):
        return remote(terms.at[block(j, share), :], got.at[slot],
                      tp_send.at[layer, j], tp_recv.at[layer, slot], tp=j)

    def down(layer, relay, hid, vd, got, with_mix):
        per_block = n_chunks // n_pairs

        def piece(b):
            def inner(i):
                relay(b * per_block + i)

            loop(per_block, inner)
            for side in (0, 1):
                j = side * n_pairs + b
                rows = block(j, share)
                value = 0.5 * jnp.dot(hid[rows, :], vd[...], preferred_element_type=F32)
                if with_mix:
                    value = value + jnp.dot(mixed[rows, :], vo[...], preferred_element_type=F32)
                terms[rows, :] = value.astype(BF16)

                @pl.when(j != t)
                def _():
                    tp_copy(layer, j, t, got).start()

        loop(n_pairs, piece)

    def reduce_tp(layer, got, start_value):
        resid[...] = start_value + terms[block(t, share), :].astype(F32)

        def add(i):
            j = (t + 1 + i) % n_tp
            tp_copy(layer, j, j, got).wait_recv()
            resid[...] = resid[...] + got[j].astype(F32)

        loop(n_tp - 1, add)

        def drain(i):
            j = (t + 1 + i) % n_tp
            tp_copy(layer, j, t, got).wait_send()

        loop(n_tp - 1, drain)

    loads[0].wait()
    loads[1].wait()
    gates_one(f)

    def pass_on(i):
        j = (f + 1 + i) % n_fs
        p0_copy(j, j).wait_recv()
        fw_copy(j).start()

    loop(n_fs - 1, pass_on)

    def other_rows(i):
        j = (f + 1 + i) % n_fs
        s1_copy(j, j).wait_recv()
        fw_in(j).wait_recv()
        gates_one(j)

    def fw_in(slot):
        start = pl.multiple_of(slot * rows_in + (1 - c_own) * half_in, half_in)
        place = raw.at[pl.ds(start, half_in), :]
        return remote(place, place, fw_send.at[slot], fw_recv.at[slot], tp=partner)

    loop(n_fs - 1, other_rows)
    relay_one, drain_one = chain(0, in1, hid1, True)
    loads[2].wait()
    loads[3].wait()
    down(0, relay_one, hid1, vd1, got1, True)
    reduce_tp(0, got1, raw[block(t, share), :].astype(F32))

    squares[f] = squares_of(resid[...])

    def sq_start(i):
        sq_copy((f + 1 + i) % n_fs, f).start()

    def sq_wait(i):
        j = (f + 1 + i) % n_fs
        sq_copy(j, j).wait_recv()

    loop(n_fs - 1, sq_start)
    drain_one()
    loop(n_fs - 1, sq_wait)
    summed = squares[0]
    for j in range(1, n_fs):
        summed = summed + squares[j]
    nb2[block(t, share), :] = (resid[...] * scale_of(summed) * gain2[:, cols(f)]).astype(BF16)

    def nrm_copy(j, slot):
        place = nb2.at[block(slot, share), :]
        return remote(place, place, nrm_send.at[j], nrm_recv.at[slot], tp=j)

    def nfw_copy(slot):
        place = nb2.at[block(slot, share), :]
        return remote(place, place, nfw_send.at[slot], nfw_recv.at[slot], tp=partner)

    def same_core(i):
        return (t + 2 + 2 * i) % n_tp

    def nrm_start(i):
        nrm_copy(same_core(i), t).start()

    loop(n_pairs - 1, nrm_start)
    nfw_copy(t).start()
    loads[4].wait()
    loads[5].wait()

    def gates_two(j):
        rows = block(j, share)
        x = nb2[rows, :]
        grads[0, rows, :] = jnp.dot(x, vg2[...], preferred_element_type=F32)
        grads[1, rows, :] = jnp.dot(x, vu2[...], preferred_element_type=F32)

    gates_two(t)
    nfw_copy(partner).wait_recv()
    gates_two(partner)

    def nrm_pass(i):
        j = same_core(i)
        nrm_copy(j, j).wait_recv()
        nfw_copy(j).start()
        gates_two(j)

    loop(n_pairs - 1, nrm_pass)

    def nrm_last(i):
        j = (partner + 2 + 2 * i) % n_tp
        nfw_copy(j).wait_recv()
        gates_two(j)

    loop(n_pairs - 1, nrm_last)
    relay_two, drain_two = chain(1, in2, hid2, False)
    loads[6].wait()
    down(1, relay_two, hid2, vd2, got2, False)
    reduce_tp(1, got2, resid[...])
    done_rows[...] = resid[...].astype(BF16)

    def out_copy(j, slot):
        return remote(done_rows, joined.at[:, cols(slot)], out_send.at[j], out_recv.at[slot], fs=t, tp=j)

    def ofw_copy(slot):
        place = joined.at[:, cols(slot)]
        return remote(place, place, ofw_send.at[slot], ofw_recv.at[slot], tp=partner)

    def out_start(i):
        j = c_own + 2 * i

        @pl.when(jnp.logical_or(f != t, j != t))
        def _():
            out_copy(j, f).start()

    loop(n_pairs, out_start)

    @pl.when(f == t)
    def _():
        joined[:, cols(f)] = done_rows[...]

    takes = c_own == f % 2

    @pl.when(takes)
    def _():
        def take(i):
            j = (f + i) % n_fs

            @pl.when(jnp.logical_or(f != t, j != f))
            def _():
                out_copy(t, j).wait_recv()

            ofw_copy(j).start()

        loop(n_fs, take)

    @pl.when(jnp.logical_not(takes))
    def _():
        def take(i):
            ofw_copy((f + i) % n_fs).wait_recv()

        loop(n_fs, take)

    out[...] = joined[...]

    drain_two()

    def last_fs(i):
        j = (f + 1 + i) % n_fs
        p0_copy(j, f).wait_send()
        fw_copy(j).wait_send()
        s1_copy(j, f).wait_send()
        sq_copy(j, f).wait_send()

    loop(n_fs - 1, last_fs)

    def last_mix(j):
        @pl.when(jnp.logical_and(j <= f, f < n_fs - 1))
        def _():
            mix_copy(j, 0, f).wait_send()

        @pl.when(jnp.logical_and(j >= f, f > 0))
        def _():
            mix_copy(j, 1, f).wait_send()

        @pl.when(takes)
        def _():
            ofw_copy(j).wait_send()

    loop(n_fs, last_mix)

    def last_nrm(i):
        nrm_copy(same_core(i), t).wait_send()

    loop(n_pairs - 1, last_nrm)

    def last_out(i):
        j = c_own + 2 * i
        nfw_copy(j).wait_send()

        @pl.when(jnp.logical_or(f != t, j != t))
        def _():
            out_copy(j, f).wait_send()

    loop(n_pairs, last_out)


def solution(mesh):
    n_fs, n_tp = mesh.shape["fs"], mesh.shape["tp"]

    def local(tokens, mix_heads, norm_first, gate_first, up_first, down_first, out_weight,
              norm_second, gate_second, up_second, down_second):
        rows_in, width = tokens.shape
        total = rows_in * n_fs
        share = total // n_tp
        dc, hidden = gate_first.shape
        heads = mix_heads.shape[1]
        chunk = rows_in // 4
        n_chunks = total // 2 // chunk
        dma = pltpu.SemaphoreType.DMA
        vmem = pl.BlockSpec(memory_space=pltpu.VMEM)
        hbm = pl.BlockSpec(memory_space=pl.ANY)
        return pl.pallas_call(
            functools.partial(kernel, n_fs, n_tp, chunk),
            out_shape=jax.ShapeDtypeStruct((rows_in, width), BF16),
            in_specs=[vmem, vmem, vmem, hbm, hbm, hbm, hbm, vmem, hbm, hbm, hbm],
            out_specs=vmem,
            scratch_shapes=[
                pltpu.VMEM(gate_first.shape, BF16),
                pltpu.VMEM(up_first.shape, BF16),
                pltpu.VMEM(down_first.shape, BF16),
                pltpu.VMEM(out_weight.shape, BF16),
                pltpu.VMEM(gate_second.shape, BF16),
                pltpu.VMEM(up_second.shape, BF16),
                pltpu.VMEM(down_second.shape, BF16),
                pltpu.VMEM((total, dc), BF16),
                pltpu.VMEM((total, dc), BF16),
                pltpu.VMEM((total, heads), BF16),
                pltpu.VMEM((2, total, hidden), F32),
                pltpu.VMEM((2, total, hidden), BF16),
                pltpu.VMEM((2, total, hidden), BF16),
                pltpu.VMEM((2, total, hidden), BF16),
                pltpu.VMEM((total, hidden), BF16),
                pltpu.VMEM((total, hidden), BF16),
                pltpu.VMEM((total, dc), BF16),
                pltpu.VMEM((n_tp, share, dc), BF16),
                pltpu.VMEM((n_tp, share, dc), BF16),
                pltpu.VMEM((share, dc), F32),
                pltpu.VMEM((n_fs, 8, rows_in), F32),
                pltpu.VMEM((n_fs, 8, share), F32),
                pltpu.VMEM((share, dc), BF16),
                pltpu.VMEM((rows_in, width), BF16),
                dma((7,)), dma((n_fs,)), dma((n_fs,)), dma((n_fs,)), dma((n_fs,)), dma((n_fs,)), dma((n_fs,)),
                dma((n_fs, 2)), dma((n_fs,)),
                dma((2, 2, n_chunks)), dma((2, 2, n_chunks)), dma((2, 2, n_chunks)), dma((2, 2, n_chunks)),
                dma((2, n_tp)), dma((2, n_tp)),
                dma((n_fs,)), dma((n_fs,)), dma((n_tp,)), dma((n_tp,)), dma((n_tp,)), dma((n_tp,)),
                dma((n_tp,)), dma((n_fs,)), dma((n_fs,)), dma((n_fs,)),
            ],
            compiler_params=pltpu.CompilerParams(
                collective_id=0, has_side_effects=True, vmem_limit_bytes=60 * 1024 * 1024),
        )(tokens, mix_heads, norm_first.reshape(1, -1), gate_first, up_first, down_first, out_weight,
          norm_second.reshape(1, -1), gate_second, up_second, down_second)

    in_specs = (
        P(("grp", "fs"), None),
        P(("grp", "fs"), "tp"),
        P(),
        P("fs", "tp"),
        P("fs", "tp"),
        P("tp", "fs"),
        P("tp", "fs"),
        P(),
        P("fs", "tp"),
        P("fs", "tp"),
        P("tp", "fs"),
    )
    return jax.shard_map(local, mesh=mesh, in_specs=in_specs, out_specs=P(("grp", "fs"), None), check_vma=False)
```

```python
import functools

import jax
import jax.numpy as jnp
from jax import lax
from jax.experimental import pallas as pl
from jax.experimental.pallas import tpu as pltpu
from jax.sharding import PartitionSpec as P

EPS = 0.1
MESH = pl.DeviceIdType.MESH
BF16 = jnp.bfloat16
F32 = jnp.float32


def loop(count, body):
    def step(i, carry):
        body(i)
        return carry

    lax.fori_loop(0, count, step, 0)


def kernel(n_fs, n_tp, chunk,
           tok, mix, gain1, wg1, wu1, wd1, wo, gain2, wg2, wu2, wd2,
           out,
           vg1, vu1, vd1, vo, vg2, vu2, vd2,
           raw, nb2, mixed, grads, sums, in1, in2, hid1, hid2,
           terms, got1, got2, resid, squares1, squares, done_rows, joined,
           wsem, p0_send, p0_recv, fw_send, fw_recv, s1_send, s1_recv, mix_send, mix_recv,
           rs_send, rs_recv, ag_send, ag_recv, tp_send, tp_recv,
           sq_send, sq_recv, nrm_send, nrm_recv, nfw_send, nfw_recv,
           out_send, out_recv, ofw_send, ofw_recv):
    f, t = lax.axis_index("fs"), lax.axis_index("tp")
    rows_in, width = tok.shape
    total = rows_in * n_fs
    share = total // n_tp
    half = total // 2
    n_chunks = half // chunk
    dc = width // n_fs

    weights = ((wg1, vg1), (wu1, vu1), (wd1, vd1), (wo, vo), (wg2, vg2), (wu2, vu2), (wd2, vd2))
    loads = [pltpu.make_async_copy(a, b, wsem.at[i]) for i, (a, b) in enumerate(weights)]
    for load in loads:
        load.start()

    barrier = pltpu.get_barrier_semaphore()

    def greet(i):
        pf, pt = i // n_tp, i % n_tp

        @pl.when(jnp.logical_or(pf != f, pt != t))
        def _():
            pl.semaphore_signal(barrier, inc=1, device_id={"fs": pf, "tp": pt}, device_id_type=MESH)

    loop(n_fs * n_tp, greet)

    def cols(j):
        return pl.ds(pl.multiple_of(j * dc, dc), dc)

    def block(j, size):
        return pl.ds(pl.multiple_of(j * size, size), size)

    def remote(src, dst, send, recv, **where):
        return pltpu.make_async_remote_copy(
            src_ref=src, dst_ref=dst, send_sem=send, recv_sem=recv,
            device_id=where, device_id_type=MESH)

    c_own = t % 2
    partner = t + 1 - 2 * c_own
    half_in = rows_in // 2
    n_pairs = n_tp // 2

    def squares_of(x):
        own = jnp.sum(x * x, axis=-1, keepdims=True)
        return jnp.transpose(jnp.broadcast_to(own, (x.shape[0], 128)))[0:8, :]

    def scale_of(summed):
        column = jnp.transpose(jnp.broadcast_to(summed[0:1, :], (128, summed.shape[1])))[:, 0:1]
        return lax.rsqrt(column * (1.0 / width) + EPS)

    def piece_of(slot):
        return pl.ds(pl.multiple_of(slot * rows_in + c_own * half_in, half_in), half_in)

    def p0_copy(j, slot):
        return remote(tok.at[block(c_own, half_in), cols(j)], raw.at[piece_of(slot), :],
                      p0_send.at[j], p0_recv.at[slot], fs=j)

    def fw_copy(slot):
        place = raw.at[piece_of(slot), :]
        return remote(place, place, fw_send.at[slot], fw_recv.at[slot], tp=partner)

    def s1_copy(j, slot):
        return remote(squares1.at[f], squares1.at[slot], s1_send.at[j], s1_recv.at[slot], fs=j)

    def sq_copy(j, slot):
        return remote(squares.at[f], squares.at[slot], sq_send.at[j], sq_recv.at[slot], fs=j)

    def mix_copy(slot, side, where):
        place = mixed.at[block(slot, rows_in), :]
        return remote(place, place, mix_send.at[slot, side], mix_recv.at[slot], fs=where)

    mixed[block(f, rows_in), :] = mix[...]
    pl.semaphore_wait(barrier, n_fs * n_tp - 1)

    def p0_start(i):
        p0_copy((f + 1 + i) % n_fs, f).start()

    loop(n_fs - 1, p0_start)
    squares1[f] = squares_of(tok[...].astype(F32))

    def s1_start(i):
        s1_copy((f + 1 + i) % n_fs, f).start()

    loop(n_fs - 1, s1_start)

    @pl.when(f < n_fs - 1)
    def _():
        mix_copy(f, 0, f + 1).start()

    @pl.when(f > 0)
    def _():
        mix_copy(f, 1, f - 1).start()

    raw[block(f, rows_in), :] = tok[:, cols(f)]

    def gates_one(j):
        rows = block(j, rows_in)
        x = (raw[rows, :].astype(F32) * scale_of(squares1[j]) * gain1[:, cols(f)]).astype(BF16)
        grads[0, rows, :] = jnp.dot(x, vg1[...], preferred_element_type=F32)
        grads[1, rows, :] = jnp.dot(x, vu1[...], preferred_element_type=F32)

    def side_of(side):
        hops = jnp.where(side == 0, n_fs - 1 - f, f)
        toward = jnp.where(side == 0, f - 1, f + 1)
        away = jnp.where(side == 0, f + 1, f - 1)
        return hops, toward, away

    near = jnp.where(2 * f >= n_fs, 0, 1)

    def chain(layer, arrived, hid, with_mix):
        def rows_of(side, c):
            return pl.ds(pl.multiple_of(side * half + c * chunk, chunk), chunk)

        def rs_copy(side, c, where):
            rows = rows_of(side, c)
            return remote(sums.at[:, rows, :], arrived.at[:, rows, :],
                          rs_send.at[layer, side, c], rs_recv.at[layer, side, c], fs=where)

        def ag_copy(side, c, where):
            rows = rows_of(side, c)
            return remote(hid.at[rows, :], hid.at[rows, :],
                          ag_send.at[layer, side, c], ag_recv.at[layer, side, c], fs=where)

        for side in (0, 1):
            hops, toward, away = side_of(side)

            @pl.when(hops == 0)
            def _():
                def first(c):
                    rows = rows_of(side, c)
                    sums[:, rows, :] = grads[:, rows, :].astype(BF16)
                    rs_copy(side, c, toward).start()

                loop(n_chunks, first)

        def step(s):
            for k in (0, 1):
                side = near if k == 0 else 1 - near
                hops, toward, away = side_of(side)
                c = s - hops

                @pl.when(jnp.logical_and(hops > 0, jnp.logical_and(c >= 0, c < n_chunks)))
                def _():
                    rows = rows_of(side, c)
                    rs_copy(side, c, f).wait_recv()

                    @pl.when(hops < n_fs - 1)
                    def _():
                        sums[:, rows, :] = (grads[:, rows, :] + arrived[:, rows, :].astype(F32)).astype(BF16)
                        rs_copy(side, c, toward).start()

                    @pl.when(hops == n_fs - 1)
                    def _():
                        g = grads[0, rows, :] + arrived[0, rows, :].astype(F32)
                        v = grads[1, rows, :] + arrived[1, rows, :].astype(F32)
                        hid[rows, :] = (g / (1.0 + jnp.exp(-g)) * v).astype(BF16)
                        ag_copy(side, c, away).start()

            if with_mix:
                @pl.when(jnp.logical_and(s > 0, s < n_fs))
                def _():
                    low, high = f - s, f + s

                    @pl.when(low >= 0)
                    def _():
                        mix_copy(low, 0, f).wait_recv()

                        @pl.when(f < n_fs - 1)
                        def _():
                            mix_copy(low, 0, f + 1).start()

                    @pl.when(high < n_fs)
                    def _():
                        mix_copy(high, 1, f).wait_recv()

                        @pl.when(f > 0)
                        def _():
                            mix_copy(high, 1, f - 1).start()

        loop(n_chunks + n_fs - 1, step)

        def relay(c):
            for k in (0, 1):
                side = 1 - near if k == 0 else near
                hops, toward, away = side_of(side)

                @pl.when(hops < n_fs - 1)
                def _():
                    ag_copy(side, c, f).wait_recv()

                    @pl.when(hops > 0)
                    def _():
                        ag_copy(side, c, away).start()

        def drain(c):
            for side in (0, 1):
                hops, toward, away = side_of(side)

                @pl.when(hops < n_fs - 1)
                def _():
                    rs_copy(side, c, f).wait_send()

                @pl.when(hops > 0)
                def _():
                    ag_copy(side, c, f).wait_send()

        return relay, lambda: loop(n_chunks, drain)

    def tp_copy(layer, j, slot, got):
        return remote(terms.at[block(j, share), :], got.at[slot],
                      tp_send.at[layer, j], tp_recv.at[layer, slot], tp=j)

    def down(layer, relay, hid, vd, got, with_mix):
        per_block = n_chunks // n_pairs

        def piece(b):
            def inner(i):
                relay(b * per_block + i)

            loop(per_block, inner)
            for side in (0, 1):
                j = side * n_pairs + b
                rows = block(j, share)
                value = 0.5 * jnp.dot(hid[rows, :], vd[...], preferred_element_type=F32)
                if with_mix:
                    value = value + jnp.dot(mixed[rows, :], vo[...], preferred_element_type=F32)
                terms[rows, :] = value.astype(BF16)

                @pl.when(j != t)
                def _():
                    tp_copy(layer, j, t, got).start()

        loop(n_pairs, piece)

    def reduce_tp(layer, got, start_value):
        resid[...] = start_value + terms[block(t, share), :].astype(F32)

        def add(i):
            j = (t + 1 + i) % n_tp
            tp_copy(layer, j, j, got).wait_recv()
            resid[...] = resid[...] + got[j].astype(F32)

        loop(n_tp - 1, add)

        def drain(i):
            j = (t + 1 + i) % n_tp
            tp_copy(layer, j, t, got).wait_send()

        loop(n_tp - 1, drain)

    loads[0].wait()
    loads[1].wait()
    gates_one(f)

    def pass_on(i):
        j = (f + 1 + i) % n_fs
        p0_copy(j, j).wait_recv()
        fw_copy(j).start()

    loop(n_fs - 1, pass_on)

    def other_rows(i):
        j = (f + 1 + i) % n_fs
        s1_copy(j, j).wait_recv()
        fw_in(j).wait_recv()
        gates_one(j)

    def fw_in(slot):
        start = pl.multiple_of(slot * rows_in + (1 - c_own) * half_in, half_in)
        place = raw.at[pl.ds(start, half_in), :]
        return remote(place, place, fw_send.at[slot], fw_recv.at[slot], tp=partner)

    loop(n_fs - 1, other_rows)
    relay_one, drain_one = chain(0, in1, hid1, True)
    loads[2].wait()
    loads[3].wait()
    down(0, relay_one, hid1, vd1, got1, True)
    reduce_tp(0, got1, raw[block(t, share), :].astype(F32))

    squares[f] = squares_of(resid[...])

    def sq_start(i):
        sq_copy((f + 1 + i) % n_fs, f).start()

    def sq_wait(i):
        j = (f + 1 + i) % n_fs
        sq_copy(j, j).wait_recv()

    loop(n_fs - 1, sq_start)
    drain_one()
    loop(n_fs - 1, sq_wait)
    summed = squares[0]
    for j in range(1, n_fs):
        summed = summed + squares[j]
    nb2[block(t, share), :] = (resid[...] * scale_of(summed) * gain2[:, cols(f)]).astype(BF16)

    def nrm_copy(j, slot):
        place = nb2.at[block(slot, share), :]
        return remote(place, place, nrm_send.at[j], nrm_recv.at[slot], tp=j)

    def nfw_copy(slot):
        place = nb2.at[block(slot, share), :]
        return remote(place, place, nfw_send.at[slot], nfw_recv.at[slot], tp=partner)

    def same_core(i):
        return (t + 2 + 2 * i) % n_tp

    def nrm_start(i):
        nrm_copy(same_core(i), t).start()

    loop(n_pairs - 1, nrm_start)
    nfw_copy(t).start()
    loads[4].wait()
    loads[5].wait()

    def gates_two(j):
        rows = block(j, share)
        x = nb2[rows, :]
        grads[0, rows, :] = jnp.dot(x, vg2[...], preferred_element_type=F32)
        grads[1, rows, :] = jnp.dot(x, vu2[...], preferred_element_type=F32)

    gates_two(t)
    nfw_copy(partner).wait_recv()
    gates_two(partner)

    def nrm_pass(i):
        j = same_core(i)
        nrm_copy(j, j).wait_recv()
        nfw_copy(j).start()
        gates_two(j)

    loop(n_pairs - 1, nrm_pass)

    def nrm_last(i):
        j = (partner + 2 + 2 * i) % n_tp
        nfw_copy(j).wait_recv()
        gates_two(j)

    loop(n_pairs - 1, nrm_last)
    relay_two, drain_two = chain(1, in2, hid2, False)
    loads[6].wait()
    down(1, relay_two, hid2, vd2, got2, False)
    reduce_tp(1, got2, resid[...])
    done_rows[...] = resid[...].astype(BF16)

    def out_copy(j, slot):
        return remote(done_rows, joined.at[:, cols(slot)], out_send.at[j], out_recv.at[slot], fs=t, tp=j)

    def ofw_copy(slot):
        place = joined.at[:, cols(slot)]
        return remote(place, place, ofw_send.at[slot], ofw_recv.at[slot], tp=partner)

    def out_start(i):
        j = c_own + 2 * i

        @pl.when(jnp.logical_or(f != t, j != t))
        def _():
            out_copy(j, f).start()

    loop(n_pairs, out_start)

    @pl.when(f == t)
    def _():
        joined[:, cols(f)] = done_rows[...]

    takes = c_own == f % 2

    @pl.when(takes)
    def _():
        def take(i):
            j = (f + i) % n_fs

            @pl.when(jnp.logical_or(f != t, j != f))
            def _():
                out_copy(t, j).wait_recv()

            ofw_copy(j).start()

        loop(n_fs, take)

    @pl.when(jnp.logical_not(takes))
    def _():
        def take(i):
            ofw_copy((f + i) % n_fs).wait_recv()

        loop(n_fs, take)

    out[...] = joined[...]

    drain_two()

    def last_fs(i):
        j = (f + 1 + i) % n_fs
        p0_copy(j, f).wait_send()
        fw_copy(j).wait_send()
        s1_copy(j, f).wait_send()
        sq_copy(j, f).wait_send()

    loop(n_fs - 1, last_fs)

    def last_mix(j):
        @pl.when(jnp.logical_and(j <= f, f < n_fs - 1))
        def _():
            mix_copy(j, 0, f).wait_send()

        @pl.when(jnp.logical_and(j >= f, f > 0))
        def _():
            mix_copy(j, 1, f).wait_send()

        @pl.when(takes)
        def _():
            ofw_copy(j).wait_send()

    loop(n_fs, last_mix)

    def last_nrm(i):
        nrm_copy(same_core(i), t).wait_send()

    loop(n_pairs - 1, last_nrm)

    def last_out(i):
        j = c_own + 2 * i
        nfw_copy(j).wait_send()

        @pl.when(jnp.logical_or(f != t, j != t))
        def _():
            out_copy(j, f).wait_send()

    loop(n_pairs, last_out)


def solution(mesh):
    n_fs, n_tp = mesh.shape["fs"], mesh.shape["tp"]

    def local(tokens, mix_heads, norm_first, gate_first, up_first, down_first, out_weight,
              norm_second, gate_second, up_second, down_second):
        rows_in, width = tokens.shape
        total = rows_in * n_fs
        share = total // n_tp
        dc, hidden = gate_first.shape
        heads = mix_heads.shape[1]
        chunk = rows_in // 2
        n_chunks = total // 2 // chunk
        dma = pltpu.SemaphoreType.DMA
        vmem = pl.BlockSpec(memory_space=pltpu.VMEM)
        hbm = pl.BlockSpec(memory_space=pl.ANY)
        return pl.pallas_call(
            functools.partial(kernel, n_fs, n_tp, chunk),
            out_shape=jax.ShapeDtypeStruct((rows_in, width), BF16),
            in_specs=[vmem, vmem, vmem, hbm, hbm, hbm, hbm, vmem, hbm, hbm, hbm],
            out_specs=vmem,
            scratch_shapes=[
                pltpu.VMEM(gate_first.shape, BF16),
                pltpu.VMEM(up_first.shape, BF16),
                pltpu.VMEM(down_first.shape, BF16),
                pltpu.VMEM(out_weight.shape, BF16),
                pltpu.VMEM(gate_second.shape, BF16),
                pltpu.VMEM(up_second.shape, BF16),
                pltpu.VMEM(down_second.shape, BF16),
                pltpu.VMEM((total, dc), BF16),
                pltpu.VMEM((total, dc), BF16),
                pltpu.VMEM((total, heads), BF16),
                pltpu.VMEM((2, total, hidden), F32),
                pltpu.VMEM((2, total, hidden), BF16),
                pltpu.VMEM((2, total, hidden), BF16),
                pltpu.VMEM((2, total, hidden), BF16),
                pltpu.VMEM((total, hidden), BF16),
                pltpu.VMEM((total, hidden), BF16),
                pltpu.VMEM((total, dc), BF16),
                pltpu.VMEM((n_tp, share, dc), BF16),
                pltpu.VMEM((n_tp, share, dc), BF16),
                pltpu.VMEM((share, dc), F32),
                pltpu.VMEM((n_fs, 8, rows_in), F32),
                pltpu.VMEM((n_fs, 8, share), F32),
                pltpu.VMEM((share, dc), BF16),
                pltpu.VMEM((rows_in, width), BF16),
                dma((7,)), dma((n_fs,)), dma((n_fs,)), dma((n_fs,)), dma((n_fs,)), dma((n_fs,)), dma((n_fs,)),
                dma((n_fs, 2)), dma((n_fs,)),
                dma((2, 2, n_chunks)), dma((2, 2, n_chunks)), dma((2, 2, n_chunks)), dma((2, 2, n_chunks)),
                dma((2, n_tp)), dma((2, n_tp)),
                dma((n_fs,)), dma((n_fs,)), dma((n_tp,)), dma((n_tp,)), dma((n_tp,)), dma((n_tp,)),
                dma((n_tp,)), dma((n_fs,)), dma((n_fs,)), dma((n_fs,)),
            ],
            compiler_params=pltpu.CompilerParams(
                collective_id=0, has_side_effects=True, vmem_limit_bytes=60 * 1024 * 1024),
        )(tokens, mix_heads, norm_first.reshape(1, -1), gate_first, up_first, down_first, out_weight,
          norm_second.reshape(1, -1), gate_second, up_second, down_second)

    in_specs = (
        P(("grp", "fs"), None),
        P(("grp", "fs"), "tp"),
        P(),
        P("fs", "tp"),
        P("fs", "tp"),
        P("tp", "fs"),
        P("tp", "fs"),
        P(),
        P("fs", "tp"),
        P("fs", "tp"),
        P("tp", "fs"),
    )
    return jax.shard_map(local, mesh=mesh, in_specs=in_specs, out_specs=P(("grp", "fs"), None), check_vma=False)
```

```python
import functools

import jax
import jax.numpy as jnp
from jax import lax
from jax.experimental import pallas as pl
from jax.experimental.pallas import tpu as pltpu
from jax.sharding import PartitionSpec as P

EPS = 0.1
MESH = pl.DeviceIdType.MESH
BF16 = jnp.bfloat16
F32 = jnp.float32


def loop(count, body):
    def step(i, carry):
        body(i)
        return carry

    lax.fori_loop(0, count, step, 0)


def kernel(n_fs, n_tp, chunk,
           tok, mix, gain1, wg1, wu1, wd1, wo, gain2, wg2, wu2, wd2,
           out,
           vg1, vu1, vd1, vo, vg2, vu2, vd2,
           raw, nb2, mixed, grads, sums, in1, in2, hid1, hid2,
           terms, got1, got2, resid, squares1, squares1_in, squares, done_rows, joined,
           wsem, p0_send, p0_recv, fw_send, fw_recv, s1_send, s1_recv, mix_send, mix_recv,
           rs_send, rs_recv, ag_send, ag_recv, tp_send, tp_recv,
           sq_send, sq_recv, nrm_send, nrm_recv, nfw_send, nfw_recv,
           out_send, out_recv, ofw_send, ofw_recv, sfw_send, sfw_recv):
    f, t = lax.axis_index("fs"), lax.axis_index("tp")
    rows_in, width = tok.shape
    total = rows_in * n_fs
    share = total // n_tp
    half = total // 2
    n_chunks = half // chunk
    dc = width // n_fs

    weights = ((wg1, vg1), (wu1, vu1), (wd1, vd1), (wo, vo), (wg2, vg2), (wu2, vu2), (wd2, vd2))
    loads = [pltpu.make_async_copy(a, b, wsem.at[i]) for i, (a, b) in enumerate(weights)]
    for load in loads:
        load.start()

    barrier = pltpu.get_barrier_semaphore()

    def greet(i):
        pf, pt = i // n_tp, i % n_tp

        @pl.when(jnp.logical_or(pf != f, pt != t))
        def _():
            pl.semaphore_signal(barrier, inc=1, device_id={"fs": pf, "tp": pt}, device_id_type=MESH)

    loop(n_fs * n_tp, greet)

    def cols(j):
        return pl.ds(pl.multiple_of(j * dc, dc), dc)

    def block(j, size):
        return pl.ds(pl.multiple_of(j * size, size), size)

    def remote(src, dst, send, recv, **where):
        return pltpu.make_async_remote_copy(
            src_ref=src, dst_ref=dst, send_sem=send, recv_sem=recv,
            device_id=where, device_id_type=MESH)

    c_own = t % 2
    partner = t + 1 - 2 * c_own
    half_in = rows_in // 2
    n_pairs = n_tp // 2

    def squares_of(x):
        own = jnp.sum(x * x, axis=-1, keepdims=True)
        return jnp.transpose(jnp.broadcast_to(own, (x.shape[0], 128)))[0:8, :]

    def scale_of(summed):
        column = jnp.transpose(jnp.broadcast_to(summed[0:1, :], (128, summed.shape[1])))[:, 0:1]
        return lax.rsqrt(column * (1.0 / width) + EPS)

    def piece_of(slot):
        return pl.ds(pl.multiple_of(slot * rows_in + c_own * half_in, half_in), half_in)

    def p0_copy(j, slot):
        return remote(tok.at[block(c_own, half_in), cols(j)], raw.at[piece_of(slot), :],
                      p0_send.at[j], p0_recv.at[slot], fs=j)

    def fw_copy(slot):
        place = raw.at[piece_of(slot), :]
        return remote(place, place, fw_send.at[slot], fw_recv.at[slot], tp=partner)

    def s1_copy(j, slot):
        return remote(squares1.at[f], squares1.at[slot], s1_send.at[j], s1_recv.at[slot], fs=j)

    def sq_copy(j, slot):
        return remote(squares.at[f], squares.at[slot], sq_send.at[j], sq_recv.at[slot], fs=j)

    def mix_copy(slot, side, where):
        place = mixed.at[block(slot, rows_in), :]
        return remote(place, place, mix_send.at[slot, side], mix_recv.at[slot], fs=where)

    mixed[block(f, rows_in), :] = mix[...]
    pl.semaphore_wait(barrier, n_fs * n_tp - 1)

    def p0_start(i):
        p0_copy((f + 1 + i) % n_fs, f).start()

    loop(n_fs - 1, p0_start)
    squares1[f] = squares_of(tok[...].astype(F32))

    def s1_start(i):
        j = (f + 1 + i) % n_fs

        @pl.when(j % 2 == c_own)
        def _():
            s1_copy(j, f).start()

    loop(n_fs - 1, s1_start)

    @pl.when(f < n_fs - 1)
    def _():
        mix_copy(f, 0, f + 1).start()

    @pl.when(f > 0)
    def _():
        mix_copy(f, 1, f - 1).start()

    raw[block(f, rows_in), :] = tok[:, cols(f)]

    def gates_one(j, sums_of):
        rows = block(j, rows_in)
        x = (raw[rows, :].astype(F32) * scale_of(sums_of[j]) * gain1[:, cols(f)]).astype(BF16)
        grads[0, rows, :] = jnp.dot(x, vg1[...], preferred_element_type=F32)
        grads[1, rows, :] = jnp.dot(x, vu1[...], preferred_element_type=F32)

    def side_of(side):
        hops = jnp.where(side == 0, n_fs - 1 - f, f)
        toward = jnp.where(side == 0, f - 1, f + 1)
        away = jnp.where(side == 0, f + 1, f - 1)
        return hops, toward, away

    near = jnp.where(2 * f >= n_fs, 0, 1)

    def chain(layer, arrived, hid, with_mix):
        def rows_of(side, c):
            return pl.ds(pl.multiple_of(side * half + c * chunk, chunk), chunk)

        def rs_copy(side, c, where):
            rows = rows_of(side, c)
            return remote(sums.at[:, rows, :], arrived.at[:, rows, :],
                          rs_send.at[layer, side, c], rs_recv.at[layer, side, c], fs=where)

        def ag_copy(side, c, where):
            rows = rows_of(side, c)
            return remote(hid.at[rows, :], hid.at[rows, :],
                          ag_send.at[layer, side, c], ag_recv.at[layer, side, c], fs=where)

        for side in (0, 1):
            hops, toward, away = side_of(side)

            @pl.when(hops == 0)
            def _():
                def first(c):
                    rows = rows_of(side, c)
                    sums[:, rows, :] = grads[:, rows, :].astype(BF16)
                    rs_copy(side, c, toward).start()

                loop(n_chunks, first)

        def step(s):
            for k in (0, 1):
                side = near if k == 0 else 1 - near
                hops, toward, away = side_of(side)
                c = s - hops

                @pl.when(jnp.logical_and(hops > 0, jnp.logical_and(c >= 0, c < n_chunks)))
                def _():
                    rows = rows_of(side, c)
                    rs_copy(side, c, f).wait_recv()

                    @pl.when(hops < n_fs - 1)
                    def _():
                        sums[:, rows, :] = (grads[:, rows, :] + arrived[:, rows, :].astype(F32)).astype(BF16)
                        rs_copy(side, c, toward).start()

                    @pl.when(hops == n_fs - 1)
                    def _():
                        g = grads[0, rows, :] + arrived[0, rows, :].astype(F32)
                        v = grads[1, rows, :] + arrived[1, rows, :].astype(F32)
                        hid[rows, :] = (g / (1.0 + jnp.exp(-g)) * v).astype(BF16)
                        ag_copy(side, c, away).start()

            if with_mix:
                @pl.when(jnp.logical_and(s > 0, s < n_fs))
                def _():
                    low, high = f - s, f + s

                    @pl.when(low >= 0)
                    def _():
                        mix_copy(low, 0, f).wait_recv()

                        @pl.when(f < n_fs - 1)
                        def _():
                            mix_copy(low, 0, f + 1).start()

                    @pl.when(high < n_fs)
                    def _():
                        mix_copy(high, 1, f).wait_recv()

                        @pl.when(f > 0)
                        def _():
                            mix_copy(high, 1, f - 1).start()

        loop(n_chunks + n_fs - 1, step)

        def relay(c):
            for k in (0, 1):
                side = 1 - near if k == 0 else near
                hops, toward, away = side_of(side)

                @pl.when(hops < n_fs - 1)
                def _():
                    ag_copy(side, c, f).wait_recv()

                    @pl.when(hops > 0)
                    def _():
                        ag_copy(side, c, away).start()

        def drain(c):
            for side in (0, 1):
                hops, toward, away = side_of(side)

                @pl.when(hops < n_fs - 1)
                def _():
                    rs_copy(side, c, f).wait_send()

                @pl.when(hops > 0)
                def _():
                    ag_copy(side, c, f).wait_send()

        return relay, lambda: loop(n_chunks, drain)

    def tp_copy(layer, j, slot, got):
        return remote(terms.at[block(j, share), :], got.at[slot],
                      tp_send.at[layer, j], tp_recv.at[layer, slot], tp=j)

    def down(layer, relay, hid, vd, got, with_mix):
        per_block = n_chunks // n_pairs

        def piece(b):
            def inner(i):
                relay(b * per_block + i)

            loop(per_block, inner)
            for side in (0, 1):
                j = side * n_pairs + b
                rows = block(j, share)
                value = 0.5 * jnp.dot(hid[rows, :], vd[...], preferred_element_type=F32)
                if with_mix:
                    value = value + jnp.dot(mixed[rows, :], vo[...], preferred_element_type=F32)
                terms[rows, :] = value.astype(BF16)

                @pl.when(j != t)
                def _():
                    tp_copy(layer, j, t, got).start()

        loop(n_pairs, piece)

    def reduce_tp(layer, got, start_value):
        resid[...] = start_value + terms[block(t, share), :].astype(F32)

        def add(i):
            j = (t + 1 + i) % n_tp
            tp_copy(layer, j, j, got).wait_recv()
            resid[...] = resid[...] + got[j].astype(F32)

        loop(n_tp - 1, add)

        def drain(i):
            j = (t + 1 + i) % n_tp
            tp_copy(layer, j, t, got).wait_send()

        loop(n_tp - 1, drain)

    loads[0].wait()
    loads[1].wait()
    gates_one(f, squares1)

    def pass_on(i):
        j = (f + 1 + i) % n_fs
        p0_copy(j, j).wait_recv()
        fw_copy(j).start()

    loop(n_fs - 1, pass_on)

    takes = c_own == f % 2
    share_sums = remote(squares1, squares1_in, sfw_send, sfw_recv, tp=partner)

    @pl.when(takes)
    def _():
        def take_sums(i):
            j = (f + 1 + i) % n_fs
            s1_copy(j, j).wait_recv()

        loop(n_fs - 1, take_sums)
        share_sums.start()
        squares1_in[...] = squares1[...]

    @pl.when(jnp.logical_not(takes))
    def _():
        share_sums.wait_recv()

    def other_rows(i):
        j = (f + 1 + i) % n_fs
        fw_in(j).wait_recv()
        gates_one(j, squares1_in)

    def fw_in(slot):
        start = pl.multiple_of(slot * rows_in + (1 - c_own) * half_in, half_in)
        place = raw.at[pl.ds(start, half_in), :]
        return remote(place, place, fw_send.at[slot], fw_recv.at[slot], tp=partner)

    loop(n_fs - 1, other_rows)
    relay_one, drain_one = chain(0, in1, hid1, True)
    loads[2].wait()
    loads[3].wait()
    down(0, relay_one, hid1, vd1, got1, True)
    reduce_tp(0, got1, raw[block(t, share), :].astype(F32))

    squares[f] = squares_of(resid[...])

    def sq_start(i):
        sq_copy((f + 1 + i) % n_fs, f).start()

    def sq_wait(i):
        j = (f + 1 + i) % n_fs
        sq_copy(j, j).wait_recv()

    loop(n_fs - 1, sq_start)
    drain_one()
    loop(n_fs - 1, sq_wait)
    summed = squares[0]
    for j in range(1, n_fs):
        summed = summed + squares[j]
    nb2[block(t, share), :] = (resid[...] * scale_of(summed) * gain2[:, cols(f)]).astype(BF16)

    def nrm_copy(j, slot):
        place = nb2.at[block(slot, share), :]
        return remote(place, place, nrm_send.at[j], nrm_recv.at[slot], tp=j)

    def nfw_copy(slot):
        place = nb2.at[block(slot, share), :]
        return remote(place, place, nfw_send.at[slot], nfw_recv.at[slot], tp=partner)

    def same_core(i):
        return (t + 2 + 2 * i) % n_tp

    def nrm_start(i):
        nrm_copy(same_core(i), t).start()

    loop(n_pairs - 1, nrm_start)
    nfw_copy(t).start()
    loads[4].wait()
    loads[5].wait()

    def gates_two(j):
        rows = block(j, share)
        x = nb2[rows, :]
        grads[0, rows, :] = jnp.dot(x, vg2[...], preferred_element_type=F32)
        grads[1, rows, :] = jnp.dot(x, vu2[...], preferred_element_type=F32)

    gates_two(t)
    nfw_copy(partner).wait_recv()
    gates_two(partner)

    def nrm_pass(i):
        j = same_core(i)
        nrm_copy(j, j).wait_recv()
        nfw_copy(j).start()
        gates_two(j)

    loop(n_pairs - 1, nrm_pass)

    def nrm_last(i):
        j = (partner + 2 + 2 * i) % n_tp
        nfw_copy(j).wait_recv()
        gates_two(j)

    loop(n_pairs - 1, nrm_last)
    relay_two, drain_two = chain(1, in2, hid2, False)
    loads[6].wait()
    down(1, relay_two, hid2, vd2, got2, False)
    reduce_tp(1, got2, resid[...])
    done_rows[...] = resid[...].astype(BF16)

    def out_copy(j, slot):
        return remote(done_rows, joined.at[:, cols(slot)], out_send.at[j], out_recv.at[slot], fs=t, tp=j)

    def ofw_copy(slot):
        place = joined.at[:, cols(slot)]
        return remote(place, place, ofw_send.at[slot], ofw_recv.at[slot], tp=partner)

    def out_start(i):
        j = c_own + 2 * i

        @pl.when(jnp.logical_or(f != t, j != t))
        def _():
            out_copy(j, f).start()

    loop(n_pairs, out_start)

    @pl.when(f == t)
    def _():
        joined[:, cols(f)] = done_rows[...]

    @pl.when(takes)
    def _():
        def take(i):
            j = (f + i) % n_fs

            @pl.when(jnp.logical_or(f != t, j != f))
            def _():
                out_copy(t, j).wait_recv()

            ofw_copy(j).start()

        loop(n_fs, take)

    @pl.when(jnp.logical_not(takes))
    def _():
        def take(i):
            ofw_copy((f + i) % n_fs).wait_recv()

        loop(n_fs, take)

    out[...] = joined[...]

    drain_two()

    def last_fs(i):
        j = (f + 1 + i) % n_fs
        p0_copy(j, f).wait_send()
        fw_copy(j).wait_send()

        @pl.when(j % 2 == c_own)
        def _():
            s1_copy(j, f).wait_send()

        sq_copy(j, f).wait_send()

    loop(n_fs - 1, last_fs)

    @pl.when(takes)
    def _():
        share_sums.wait_send()

    def last_mix(j):
        @pl.when(jnp.logical_and(j <= f, f < n_fs - 1))
        def _():
            mix_copy(j, 0, f).wait_send()

        @pl.when(jnp.logical_and(j >= f, f > 0))
        def _():
            mix_copy(j, 1, f).wait_send()

        @pl.when(takes)
        def _():
            ofw_copy(j).wait_send()

    loop(n_fs, last_mix)

    def last_nrm(i):
        nrm_copy(same_core(i), t).wait_send()

    loop(n_pairs - 1, last_nrm)

    def last_out(i):
        j = c_own + 2 * i
        nfw_copy(j).wait_send()

        @pl.when(jnp.logical_or(f != t, j != t))
        def _():
            out_copy(j, f).wait_send()

    loop(n_pairs, last_out)


def solution(mesh):
    n_fs, n_tp = mesh.shape["fs"], mesh.shape["tp"]

    def local(tokens, mix_heads, norm_first, gate_first, up_first, down_first, out_weight,
              norm_second, gate_second, up_second, down_second):
        rows_in, width = tokens.shape
        total = rows_in * n_fs
        share = total // n_tp
        dc, hidden = gate_first.shape
        heads = mix_heads.shape[1]
        chunk = rows_in // 2
        n_chunks = total // 2 // chunk
        dma = pltpu.SemaphoreType.DMA
        vmem = pl.BlockSpec(memory_space=pltpu.VMEM)
        hbm = pl.BlockSpec(memory_space=pl.ANY)
        return pl.pallas_call(
            functools.partial(kernel, n_fs, n_tp, chunk),
            out_shape=jax.ShapeDtypeStruct((rows_in, width), BF16),
            in_specs=[vmem, vmem, vmem, hbm, hbm, hbm, hbm, vmem, hbm, hbm, hbm],
            out_specs=vmem,
            scratch_shapes=[
                pltpu.VMEM(gate_first.shape, BF16),
                pltpu.VMEM(up_first.shape, BF16),
                pltpu.VMEM(down_first.shape, BF16),
                pltpu.VMEM(out_weight.shape, BF16),
                pltpu.VMEM(gate_second.shape, BF16),
                pltpu.VMEM(up_second.shape, BF16),
                pltpu.VMEM(down_second.shape, BF16),
                pltpu.VMEM((total, dc), BF16),
                pltpu.VMEM((total, dc), BF16),
                pltpu.VMEM((total, heads), BF16),
                pltpu.VMEM((2, total, hidden), F32),
                pltpu.VMEM((2, total, hidden), BF16),
                pltpu.VMEM((2, total, hidden), BF16),
                pltpu.VMEM((2, total, hidden), BF16),
                pltpu.VMEM((total, hidden), BF16),
                pltpu.VMEM((total, hidden), BF16),
                pltpu.VMEM((total, dc), BF16),
                pltpu.VMEM((n_tp, share, dc), BF16),
                pltpu.VMEM((n_tp, share, dc), BF16),
                pltpu.VMEM((share, dc), F32),
                pltpu.VMEM((n_fs, 8, rows_in), F32),
                pltpu.VMEM((n_fs, 8, rows_in), F32),
                pltpu.VMEM((n_fs, 8, share), F32),
                pltpu.VMEM((share, dc), BF16),
                pltpu.VMEM((rows_in, width), BF16),
                dma((7,)), dma((n_fs,)), dma((n_fs,)), dma((n_fs,)), dma((n_fs,)), dma((n_fs,)), dma((n_fs,)),
                dma((n_fs, 2)), dma((n_fs,)),
                dma((2, 2, n_chunks)), dma((2, 2, n_chunks)), dma((2, 2, n_chunks)), dma((2, 2, n_chunks)),
                dma((2, n_tp)), dma((2, n_tp)),
                dma((n_fs,)), dma((n_fs,)), dma((n_tp,)), dma((n_tp,)), dma((n_tp,)), dma((n_tp,)),
                dma((n_tp,)), dma((n_fs,)), dma((n_fs,)), dma((n_fs,)), dma, dma,
            ],
            compiler_params=pltpu.CompilerParams(
                collective_id=0, has_side_effects=True, vmem_limit_bytes=60 * 1024 * 1024),
        )(tokens, mix_heads, norm_first.reshape(1, -1), gate_first, up_first, down_first, out_weight,
          norm_second.reshape(1, -1), gate_second, up_second, down_second)

    in_specs = (
        P(("grp", "fs"), None),
        P(("grp", "fs"), "tp"),
        P(),
        P("fs", "tp"),
        P("fs", "tp"),
        P("tp", "fs"),
        P("tp", "fs"),
        P(),
        P("fs", "tp"),
        P("fs", "tp"),
        P("tp", "fs"),
    )
    return jax.shard_map(local, mesh=mesh, in_specs=in_specs, out_specs=P(("grp", "fs"), None), check_vma=False)
```

```python
import functools

import jax
import jax.numpy as jnp
from jax import lax
from jax.experimental import pallas as pl
from jax.experimental.pallas import tpu as pltpu
from jax.sharding import PartitionSpec as P

EPS = 0.1
MESH = pl.DeviceIdType.MESH
BF16 = jnp.bfloat16
F32 = jnp.float32


def loop(count, body):
    def step(i, carry):
        body(i)
        return carry

    lax.fori_loop(0, count, step, 0)


def kernel(n_fs, n_tp, chunk,
           tok, mix, gain1, wg1, wu1, wd1, wo, gain2, wg2, wu2, wd2,
           out,
           vg1, vu1, vd1, vo, vg2, vu2, vd2,
           raw, nb2, mixed, grads, sums, in1, in2, hid1, hid2,
           terms, got1, got2, resid, squares1, squares, done_rows, joined,
           wsem, p0_send, p0_recv, fw_send, fw_recv, s1_send, s1_recv, mix_send, mix_recv,
           rs_send, rs_recv, ag_send, ag_recv, tp_send, tp_recv,
           sq_send, sq_recv, nrm_send, nrm_recv, nfw_send, nfw_recv,
           out_send, out_recv, ofw_send, ofw_recv):
    f, t = lax.axis_index("fs"), lax.axis_index("tp")
    rows_in, width = tok.shape
    total = rows_in * n_fs
    share = total // n_tp
    half = total // 2
    n_chunks = half // chunk
    dc = width // n_fs

    weights = ((wg1, vg1), (wu1, vu1), (wd1, vd1), (wo, vo), (wg2, vg2), (wu2, vu2), (wd2, vd2))
    loads = [pltpu.make_async_copy(a, b, wsem.at[i]) for i, (a, b) in enumerate(weights)]
    for load in loads:
        load.start()

    barrier = pltpu.get_barrier_semaphore()

    def greet(i):
        pf, pt = i // n_tp, i % n_tp

        @pl.when(jnp.logical_or(pf != f, pt != t))
        def _():
            pl.semaphore_signal(barrier, inc=1, device_id={"fs": pf, "tp": pt}, device_id_type=MESH)

    loop(n_fs * n_tp, greet)

    def cols(j):
        return pl.ds(pl.multiple_of(j * dc, dc), dc)

    def block(j, size):
        return pl.ds(pl.multiple_of(j * size, size), size)

    def remote(src, dst, send, recv, **where):
        return pltpu.make_async_remote_copy(
            src_ref=src, dst_ref=dst, send_sem=send, recv_sem=recv,
            device_id=where, device_id_type=MESH)

    c_own = t % 2
    partner = t + 1 - 2 * c_own
    half_in = rows_in // 2
    n_pairs = n_tp // 2

    def squares_of(x):
        own = jnp.sum(x * x, axis=-1, keepdims=True)
        return jnp.transpose(jnp.broadcast_to(own, (x.shape[0], 128)))[0:8, :]

    def scale_of(summed):
        column = jnp.transpose(jnp.broadcast_to(summed[0:1, :], (128, summed.shape[1])))[:, 0:1]
        return lax.rsqrt(column * (1.0 / width) + EPS)

    def piece_of(slot):
        return pl.ds(pl.multiple_of(slot * rows_in + c_own * half_in, half_in), half_in)

    def p0_copy(j, slot):
        return remote(tok.at[block(c_own, half_in), cols(j)], raw.at[piece_of(slot), :],
                      p0_send.at[j], p0_recv.at[slot], fs=j)

    def fw_copy(slot):
        place = raw.at[piece_of(slot), :]
        return remote(place, place, fw_send.at[slot], fw_recv.at[slot], tp=partner)

    def s1_copy(j, slot):
        return remote(squares1.at[f], squares1.at[slot], s1_send.at[j], s1_recv.at[slot], fs=j)

    def sq_copy(j, slot):
        return remote(squares.at[f], squares.at[slot], sq_send.at[j], sq_recv.at[slot], fs=j)

    def mix_copy(slot, side, where):
        place = mixed.at[block(slot, rows_in), :]
        return remote(place, place, mix_send.at[slot, side], mix_recv.at[slot], fs=where)

    mixed[block(f, rows_in), :] = mix[...]
    pl.semaphore_wait(barrier, n_fs * n_tp - 1)

    def p0_start(i):
        p0_copy((f + 1 + i) % n_fs, f).start()

    loop(n_fs - 1, p0_start)
    squares1[f] = squares_of(tok[...].astype(F32))

    def s1_start(i):
        s1_copy((f + 1 + i) % n_fs, f).start()

    loop(n_fs - 1, s1_start)

    @pl.when(jnp.logical_and(f > 0, f < n_fs - 1))
    def _():
        mix_copy(f, 0, f + 1).start()
        mix_copy(f, 1, f - 1).start()

    raw[block(f, rows_in), :] = tok[:, cols(f)]

    def gates_one(j):
        rows = block(j, rows_in)
        x = (raw[rows, :].astype(F32) * scale_of(squares1[j]) * gain1[:, cols(f)]).astype(BF16)
        grads[0, rows, :] = jnp.dot(x, vg1[...], preferred_element_type=F32)
        grads[1, rows, :] = jnp.dot(x, vu1[...], preferred_element_type=F32)

    def side_of(side):
        hops = jnp.where(side == 0, n_fs - 1 - f, f)
        toward = jnp.where(side == 0, f - 1, f + 1)
        away = jnp.where(side == 0, f + 1, f - 1)
        return hops, toward, away

    near = jnp.where(2 * f >= n_fs, 0, 1)

    def chain(layer, arrived, hid, with_mix):
        def rows_of(side, c):
            return pl.ds(pl.multiple_of(side * half + c * chunk, chunk), chunk)

        def rs_copy(side, c, where):
            rows = rows_of(side, c)
            return remote(sums.at[:, rows, :], arrived.at[:, rows, :],
                          rs_send.at[layer, side, c], rs_recv.at[layer, side, c], fs=where)

        def ag_copy(side, c, where):
            rows = rows_of(side, c)
            return remote(hid.at[rows, :], hid.at[rows, :],
                          ag_send.at[layer, side, c], ag_recv.at[layer, side, c], fs=where)

        for side in (0, 1):
            hops, toward, away = side_of(side)

            @pl.when(hops == 0)
            def _():
                def first(c):
                    rows = rows_of(side, c)
                    sums[:, rows, :] = grads[:, rows, :].astype(BF16)
                    rs_copy(side, c, toward).start()

                loop(n_chunks, first)
                if with_mix:
                    mix_copy(f, 1 - side, toward).start()

        def step(s):
            for k in (0, 1):
                side = near if k == 0 else 1 - near
                hops, toward, away = side_of(side)
                c = s - hops

                @pl.when(jnp.logical_and(hops > 0, jnp.logical_and(c >= 0, c < n_chunks)))
                def _():
                    rows = rows_of(side, c)
                    rs_copy(side, c, f).wait_recv()

                    @pl.when(hops < n_fs - 1)
                    def _():
                        sums[:, rows, :] = (grads[:, rows, :] + arrived[:, rows, :].astype(F32)).astype(BF16)
                        rs_copy(side, c, toward).start()

                    @pl.when(hops == n_fs - 1)
                    def _():
                        g = grads[0, rows, :] + arrived[0, rows, :].astype(F32)
                        v = grads[1, rows, :] + arrived[1, rows, :].astype(F32)
                        hid[rows, :] = (g / (1.0 + jnp.exp(-g)) * v).astype(BF16)
                        ag_copy(side, c, away).start()

        loop(n_chunks + n_fs - 1, step)

        def mix_step(s):
            @pl.when(jnp.logical_and(s > 0, s < n_fs))
            def _():
                low, high = f - s, f + s

                @pl.when(low >= 0)
                def _():
                    mix_copy(low, 0, f).wait_recv()

                    @pl.when(f < n_fs - 1)
                    def _():
                        mix_copy(low, 0, f + 1).start()

                @pl.when(high < n_fs)
                def _():
                    mix_copy(high, 1, f).wait_recv()

                    @pl.when(f > 0)
                    def _():
                        mix_copy(high, 1, f - 1).start()

        if with_mix:
            loop(n_fs, mix_step)

        def relay(c):
            for k in (0, 1):
                side = 1 - near if k == 0 else near
                hops, toward, away = side_of(side)

                @pl.when(hops < n_fs - 1)
                def _():
                    ag_copy(side, c, f).wait_recv()

                    @pl.when(hops > 0)
                    def _():
                        ag_copy(side, c, away).start()

        def drain(c):
            for side in (0, 1):
                hops, toward, away = side_of(side)

                @pl.when(hops < n_fs - 1)
                def _():
                    rs_copy(side, c, f).wait_send()

                @pl.when(hops > 0)
                def _():
                    ag_copy(side, c, f).wait_send()

        return relay, lambda: loop(n_chunks, drain)

    def tp_copy(layer, j, slot, got):
        return remote(terms.at[block(j, share), :], got.at[slot],
                      tp_send.at[layer, j], tp_recv.at[layer, slot], tp=j)

    def down(layer, relay, hid, vd, got, with_mix):
        per_block = n_chunks // n_pairs

        def piece(b):
            def inner(i):
                relay(b * per_block + i)

            loop(per_block, inner)
            for side in (0, 1):
                j = side * n_pairs + b
                rows = block(j, share)
                value = 0.5 * jnp.dot(hid[rows, :], vd[...], preferred_element_type=F32)
                if with_mix:
                    value = value + jnp.dot(mixed[rows, :], vo[...], preferred_element_type=F32)
                terms[rows, :] = value.astype(BF16)

                @pl.when(j != t)
                def _():
                    tp_copy(layer, j, t, got).start()

        loop(n_pairs, piece)

    def reduce_tp(layer, got, start_value):
        resid[...] = start_value + terms[block(t, share), :].astype(F32)

        def add(i):
            j = (t + 1 + i) % n_tp
            tp_copy(layer, j, j, got).wait_recv()
            resid[...] = resid[...] + got[j].astype(F32)

        loop(n_tp - 1, add)

        def drain(i):
            j = (t + 1 + i) % n_tp
            tp_copy(layer, j, t, got).wait_send()

        loop(n_tp - 1, drain)

    loads[0].wait()
    loads[1].wait()
    gates_one(f)

    def pass_on(i):
        j = (f + 1 + i) % n_fs
        p0_copy(j, j).wait_recv()
        fw_copy(j).start()

    loop(n_fs - 1, pass_on)

    def other_rows(i):
        j = (f + 1 + i) % n_fs
        s1_copy(j, j).wait_recv()
        fw_in(j).wait_recv()
        gates_one(j)

    def fw_in(slot):
        start = pl.multiple_of(slot * rows_in + (1 - c_own) * half_in, half_in)
        place = raw.at[pl.ds(start, half_in), :]
        return remote(place, place, fw_send.at[slot], fw_recv.at[slot], tp=partner)

    loop(n_fs - 1, other_rows)
    relay_one, drain_one = chain(0, in1, hid1, True)
    loads[2].wait()
    loads[3].wait()
    down(0, relay_one, hid1, vd1, got1, True)
    reduce_tp(0, got1, raw[block(t, share), :].astype(F32))

    squares[f] = squares_of(resid[...])

    def sq_start(i):
        sq_copy((f + 1 + i) % n_fs, f).start()

    def sq_wait(i):
        j = (f + 1 + i) % n_fs
        sq_copy(j, j).wait_recv()

    loop(n_fs - 1, sq_start)
    drain_one()
    loop(n_fs - 1, sq_wait)
    summed = squares[0]
    for j in range(1, n_fs):
        summed = summed + squares[j]
    nb2[block(t, share), :] = (resid[...] * scale_of(summed) * gain2[:, cols(f)]).astype(BF16)

    def nrm_copy(j, slot):
        place = nb2.at[block(slot, share), :]
        return remote(place, place, nrm_send.at[j], nrm_recv.at[slot], tp=j)

    def nfw_copy(slot):
        place = nb2.at[block(slot, share), :]
        return remote(place, place, nfw_send.at[slot], nfw_recv.at[slot], tp=partner)

    def same_core(i):
        return (t + 2 + 2 * i) % n_tp

    def nrm_start(i):
        nrm_copy(same_core(i), t).start()

    loop(n_pairs - 1, nrm_start)
    nfw_copy(t).start()
    loads[4].wait()
    loads[5].wait()

    def gates_two(j):
        rows = block(j, share)
        x = nb2[rows, :]
        grads[0, rows, :] = jnp.dot(x, vg2[...], preferred_element_type=F32)
        grads[1, rows, :] = jnp.dot(x, vu2[...], preferred_element_type=F32)

    gates_two(t)
    nfw_copy(partner).wait_recv()
    gates_two(partner)

    def nrm_pass(i):
        j = same_core(i)
        nrm_copy(j, j).wait_recv()
        nfw_copy(j).start()
        gates_two(j)

    loop(n_pairs - 1, nrm_pass)

    def nrm_last(i):
        j = (partner + 2 + 2 * i) % n_tp
        nfw_copy(j).wait_recv()
        gates_two(j)

    loop(n_pairs - 1, nrm_last)
    relay_two, drain_two = chain(1, in2, hid2, False)
    loads[6].wait()
    down(1, relay_two, hid2, vd2, got2, False)
    reduce_tp(1, got2, resid[...])
    done_rows[...] = resid[...].astype(BF16)

    def out_copy(j, slot):
        return remote(done_rows, joined.at[:, cols(slot)], out_send.at[j], out_recv.at[slot], fs=t, tp=j)

    def ofw_copy(slot):
        place = joined.at[:, cols(slot)]
        return remote(place, place, ofw_send.at[slot], ofw_recv.at[slot], tp=partner)

    def out_start(i):
        j = c_own + 2 * i

        @pl.when(jnp.logical_or(f != t, j != t))
        def _():
            out_copy(j, f).start()

    loop(n_pairs, out_start)

    @pl.when(f == t)
    def _():
        joined[:, cols(f)] = done_rows[...]

    takes = c_own == f % 2

    @pl.when(takes)
    def _():
        def take(i):
            j = (f + i) % n_fs

            @pl.when(jnp.logical_or(f != t, j != f))
            def _():
                out_copy(t, j).wait_recv()

            ofw_copy(j).start()

        loop(n_fs, take)

    @pl.when(jnp.logical_not(takes))
    def _():
        def take(i):
            ofw_copy((f + i) % n_fs).wait_recv()

        loop(n_fs, take)

    out[...] = joined[...]

    drain_two()

    def last_fs(i):
        j = (f + 1 + i) % n_fs
        p0_copy(j, f).wait_send()
        fw_copy(j).wait_send()
        s1_copy(j, f).wait_send()
        sq_copy(j, f).wait_send()

    loop(n_fs - 1, last_fs)

    def last_mix(j):
        @pl.when(jnp.logical_and(j <= f, f < n_fs - 1))
        def _():
            mix_copy(j, 0, f).wait_send()

        @pl.when(jnp.logical_and(j >= f, f > 0))
        def _():
            mix_copy(j, 1, f).wait_send()

        @pl.when(takes)
        def _():
            ofw_copy(j).wait_send()

    loop(n_fs, last_mix)

    def last_nrm(i):
        nrm_copy(same_core(i), t).wait_send()

    loop(n_pairs - 1, last_nrm)

    def last_out(i):
        j = c_own + 2 * i
        nfw_copy(j).wait_send()

        @pl.when(jnp.logical_or(f != t, j != t))
        def _():
            out_copy(j, f).wait_send()

    loop(n_pairs, last_out)


def solution(mesh):
    n_fs, n_tp = mesh.shape["fs"], mesh.shape["tp"]

    def local(tokens, mix_heads, norm_first, gate_first, up_first, down_first, out_weight,
              norm_second, gate_second, up_second, down_second):
        rows_in, width = tokens.shape
        total = rows_in * n_fs
        share = total // n_tp
        dc, hidden = gate_first.shape
        heads = mix_heads.shape[1]
        chunk = rows_in // 2
        n_chunks = total // 2 // chunk
        dma = pltpu.SemaphoreType.DMA
        vmem = pl.BlockSpec(memory_space=pltpu.VMEM)
        hbm = pl.BlockSpec(memory_space=pl.ANY)
        return pl.pallas_call(
            functools.partial(kernel, n_fs, n_tp, chunk),
            out_shape=jax.ShapeDtypeStruct((rows_in, width), BF16),
            in_specs=[vmem, vmem, vmem, hbm, hbm, hbm, hbm, vmem, hbm, hbm, hbm],
            out_specs=vmem,
            scratch_shapes=[
                pltpu.VMEM(gate_first.shape, BF16),
                pltpu.VMEM(up_first.shape, BF16),
                pltpu.VMEM(down_first.shape, BF16),
                pltpu.VMEM(out_weight.shape, BF16),
                pltpu.VMEM(gate_second.shape, BF16),
                pltpu.VMEM(up_second.shape, BF16),
                pltpu.VMEM(down_second.shape, BF16),
                pltpu.VMEM((total, dc), BF16),
                pltpu.VMEM((total, dc), BF16),
                pltpu.VMEM((total, heads), BF16),
                pltpu.VMEM((2, total, hidden), F32),
                pltpu.VMEM((2, total, hidden), BF16),
                pltpu.VMEM((2, total, hidden), BF16),
                pltpu.VMEM((2, total, hidden), BF16),
                pltpu.VMEM((total, hidden), BF16),
                pltpu.VMEM((total, hidden), BF16),
                pltpu.VMEM((total, dc), BF16),
                pltpu.VMEM((n_tp, share, dc), BF16),
                pltpu.VMEM((n_tp, share, dc), BF16),
                pltpu.VMEM((share, dc), F32),
                pltpu.VMEM((n_fs, 8, rows_in), F32),
                pltpu.VMEM((n_fs, 8, share), F32),
                pltpu.VMEM((share, dc), BF16),
                pltpu.VMEM((rows_in, width), BF16),
                dma((7,)), dma((n_fs,)), dma((n_fs,)), dma((n_fs,)), dma((n_fs,)), dma((n_fs,)), dma((n_fs,)),
                dma((n_fs, 2)), dma((n_fs,)),
                dma((2, 2, n_chunks)), dma((2, 2, n_chunks)), dma((2, 2, n_chunks)), dma((2, 2, n_chunks)),
                dma((2, n_tp)), dma((2, n_tp)),
                dma((n_fs,)), dma((n_fs,)), dma((n_tp,)), dma((n_tp,)), dma((n_tp,)), dma((n_tp,)),
                dma((n_tp,)), dma((n_fs,)), dma((n_fs,)), dma((n_fs,)),
            ],
            compiler_params=pltpu.CompilerParams(
                collective_id=0, has_side_effects=True, vmem_limit_bytes=60 * 1024 * 1024),
        )(tokens, mix_heads, norm_first.reshape(1, -1), gate_first, up_first, down_first, out_weight,
          norm_second.reshape(1, -1), gate_second, up_second, down_second)

    in_specs = (
        P(("grp", "fs"), None),
        P(("grp", "fs"), "tp"),
        P(),
        P("fs", "tp"),
        P("fs", "tp"),
        P("tp", "fs"),
        P("tp", "fs"),
        P(),
        P("fs", "tp"),
        P("fs", "tp"),
        P("tp", "fs"),
    )
    return jax.shard_map(local, mesh=mesh, in_specs=in_specs, out_specs=P(("grp", "fs"), None), check_vma=False)
```
